32 devices in a mesh: fs: 16 (over z, y, x), tp: 2 (over core).
Axes of the slice: x: 2, y: 2, z: 4, core: 2. Of those that a mesh axis runs over, the one named last changes fastest.
Arguments:
- inputs: bfloat16 [4096, 2048], P('fs'), may hold values from -6 to 6
- query_cot: bfloat16 [4096, 1024], P('fs', 'tp'), may hold values from -0.09375 to 0.09375
- query_basis: bfloat16 [2048, 256], P('fs'), may hold values from -0.125 to 0.125
- query_master: float32 [2048, 1024], P('fs', 'tp'), may hold values from -3 to 3
- query_first: float32 [256, 1024], P('fs', 'tp'), may hold values from -4 to 4
- query_second: float32 [256, 1024], P('fs', 'tp'), may hold values from 0.02 to 4
Outputs:
- query_step: float32 [2048, 1024], P('fs', 'tp')
- query_first_new: float32 [256, 1024], P('fs', 'tp')
- query_second_new: float32 [256, 1024], P('fs', 'tp')
- query_copy: bfloat16 [2048, 1024], P('fs', 'tp')
The draws below stay inside these ranges and needn't reach their ends.
All inputs are finite; a program needn't handle non-finite values.
Results may differ from the reference program's by a relative error of at most 0.0011.
Values may be sent and summed in bfloat16 or wider, within the bound.
A program may use at most 64 MiB of HBM per device.

```python
import math
import jax
import jax.numpy as jnp
from jax import lax

D = 2048
HEADS = 8
DQK = 128
RANK = 256
TOK_DEV = 256
TOKENS = 4096
NQ = 1024
N_FS = 16


def levels(key, extent, pieces, least, top_value):
    def one(position, blocks):
        heights = jax.random.uniform(jax.random.fold_in(jax.random.fold_in(key, 6), position), (blocks,), jnp.float32, least / len(pieces), top_value / len(pieces))
        return jnp.repeat(jnp.exp(heights), extent[position] // blocks).reshape((-1,) + (1,) * (len(extent) - position - 1))

    level = one(*pieces[0])
    for cut in pieces[1:]:
        level = level * one(*cut)
    return level


def scatter_about(rng, dims, spread, reach, pieces=(), dtype=jnp.bfloat16):
    values = jax.random.normal(rng, dims, jnp.float32) * spread
    if len(pieces) > 0:
        values = levels(rng, dims, pieces, -0.22, 0.18) * values
    return jnp.clip(values, min=-reach, max=reach).astype(dtype)


def setup_inputs(seed: int = 0) -> dict:
    streams_of = jax.random.split(jax.random.key(seed), 7)
    return {
        "inputs": scatter_about(streams_of[0], (TOKENS, D), 1.0, 6.0, ((0, 16),)),
        "query_cot": scatter_about(streams_of[1], (TOKENS, NQ), (1.0 / (TOK_DEV * N_FS) ** 0.5), 0.09375, ((0, 16), (1, 2))),
        "query_basis": scatter_about(streams_of[2], (D, RANK), D ** -0.5, 0.125, ((0, 16),)),
        "query_master": scatter_about(streams_of[3], (D, NQ), 0.5, 3.0, ((0, 16), (1, 2)), jnp.float32),
        "query_first": scatter_about(streams_of[4], (RANK, NQ), 1.0, 4.0, ((0, 16), (1, 2)), jnp.float32),
        "query_second": jnp.clip(jnp.exp(math.log(4.0) - 5.2983174 * jax.random.uniform(streams_of[5], (RANK, NQ), jnp.float32) ** levels(streams_of[5], (RANK, NQ), ((0, 16), (1, 2)), -0.2, 0.2)), 0.02, 4.0),
    }


def moments(first, second, low_grad):
    first_new = 0.8 * first + 0.2 * low_grad
    second_new = 0.9 * second + 0.1 * low_grad * low_grad
    return (first_new, second_new, first_new / jnp.sqrt(second_new))

def scaled(update, width):
    shaped = update.reshape(RANK, HEADS, width)
    head_mean = lax.optimization_barrier(jnp.mean(shaped * shaped, axis=(0, 2)))
    whole_mean = jnp.mean(update * update)
    factor = 1.0 / jnp.sqrt(head_mean + whole_mean)
    return (shaped * factor[None, :, None]).reshape(RANK, HEADS * width)

def reference(inputs, query_cot, query_basis, query_master, query_first, query_second):
    gradient = jnp.dot(inputs.T, query_cot, preferred_element_type=jnp.float32)
    basis_wide = query_basis.astype(jnp.float32)
    low_grad = jnp.dot(basis_wide.T, gradient, precision=lax.Precision.HIGHEST)
    first_new, second_new, update = moments(query_first, query_second, low_grad)
    step_full = jnp.dot(basis_wide, scaled(update, DQK), precision=lax.Precision.HIGHEST)
    copy_new = (query_master + step_full).astype(jnp.bfloat16)
    return (step_full, first_new, second_new, copy_new)
```

```python
import functools

import jax
import jax.numpy as jnp
from jax import lax
from jax.experimental import pallas as pl
from jax.experimental.pallas import tpu as pltpu
from jax.sharding import PartitionSpec as P

DQK = 128
MESH = pl.DeviceIdType.MESH
CONTRACT = (((0,), (0,)), ((), ()))


def split2(value):
    high = value.astype(jnp.bfloat16)
    low = (value - high.astype(jnp.float32)).astype(jnp.bfloat16)
    return high, low


def kernel(
    n, nz, nq, tp,
    inputs_ref, cot_ref, basis_ref, master_ref, first_ref, second_ref,
    step_ref, first_out, second_out, copy_ref,
    xv, cv, mv, ball, pbuf, part, rbuf, zsend, zbuf, ubuf, ufull, sums,
    load_sem, b_send, b_recv, p_send, p_recv, r_send, r_recv, z_send, z_recv,
    u_send, u_recv, s_send, s_recv,
):
    me = lax.axis_index("fs")
    t = lax.axis_index("tp")
    z, q = me // nq, me % nq
    half = t % 2
    partner = t + 1 - 2 * half
    rank_half = ball.shape[2]
    rr, cols = first_ref.shape
    rank = rr * n
    nzh = nz // 2

    def remote(src, dst, send, recv, fs, core):
        return pltpu.make_async_remote_copy(
            src_ref=src, dst_ref=dst, send_sem=send, recv_sem=recv,
            device_id=(fs, core), device_id_type=MESH,
        )

    loads = [
        pltpu.make_async_copy(inputs_ref, xv, load_sem.at[0]),
        pltpu.make_async_copy(cot_ref, cv, load_sem.at[1]),
        pltpu.make_async_copy(master_ref, mv, load_sem.at[2]),
    ]
    for load in loads:
        load.start()

    barrier = pltpu.get_barrier_semaphore()
    for d in range(1, nz):
        pl.semaphore_signal(barrier, inc=1, device_id=((z + d) % nz * nq + q, t), device_id_type=MESH)
    for d in range(1, nq):
        pl.semaphore_signal(barrier, inc=1, device_id=(z * nq + (q + d) % nq, t), device_id_type=MESH)
    for d in range(1, tp):
        pl.semaphore_signal(barrier, inc=1, device_id=(me, (t + d) % tp), device_id_type=MESH)
    pl.semaphore_wait(barrier, nz - 1 + nq - 1 + tp - 1)

    def gather(own, buf, send, recv):
        started = []
        for d in range(1, nz):
            copy = remote(own, buf.at[me], send.at[d], recv.at[me], (z + d) % nz * nq + q, t)
            copy.start()
            started.append(copy)
        for k in range(nz):
            c = (z + k) % nz * nq + q
            if k > 0:
                remote(own, buf.at[c], send.at[0], recv.at[c], me, t).wait_recv()
            source = own if k == 0 else buf.at[c]
            for d in range(1, nq):
                copy = remote(
                    source, buf.at[c], send.at[nz + k * nq + d], recv.at[c], z * nq + (q + d) % nq, t
                )
                copy.start()
                started.append(copy)
        for k in range(nz):
            for d in range(1, nq):
                c = (z + k) % nz * nq + (q + d) % nq
                remote(own, buf.at[c], send.at[0], recv.at[c], me, t).wait_recv()
        return started

    started = []
    own_basis = basis_ref.at[:, pl.ds(pl.multiple_of(half * rank_half, rank_half), rank_half)]
    mine = pltpu.make_async_copy(own_basis, ball.at[me], load_sem.at[3])
    mine.start()
    mine.wait()
    started += gather(ball.at[me], ball, b_send, b_recv)

    loads[0].wait()
    pbuf[half] = jnp.dot(
        xv[...], ball[...].reshape(xv.shape[1], rank_half), preferred_element_type=jnp.float32
    )
    swap = remote(pbuf.at[half], pbuf.at[half], p_send, p_recv, me, partner)
    swap.start()
    started.append(swap)
    loads[1].wait()

    def shares(hh, slot):
        high, low = split2(pbuf[hh])
        value = lax.dot_general(high, cv[...], CONTRACT, preferred_element_type=jnp.float32)
        value += lax.dot_general(low, cv[...], CONTRACT, preferred_element_type=jnp.float32)
        for k in range(nzh):
            for j in range(nq):
                at = (k * nq + j) * rr
                part[j, hh * nzh + k] = value[at : at + rr].astype(part.dtype)
        for d in range(1, nq):
            to = (q + d) % nq
            copy = remote(
                part.at[to, pl.ds(hh * nzh, nzh)], rbuf.at[q, pl.ds(hh * nzh, nzh)],
                r_send.at[slot, d], r_recv.at[slot, q], z * nq + to, t,
            )
            copy.start()
            started.append(copy)

    def combine(hh, slot):
        for d in range(1, nq):
            j = (q + d) % nq
            remote(
                part.at[j, pl.ds(hh * nzh, nzh)], rbuf.at[j, pl.ds(hh * nzh, nzh)],
                r_send.at[slot, 0], r_recv.at[slot, j], me, t,
            ).wait_recv()
        for k in range(nzh):
            zz = hh * nzh + k
            total = part[q, zz].astype(jnp.float32)
            for d in range(1, nq):
                total += rbuf[(q + d) % nq, zz].astype(jnp.float32)
            zsend[zz] = total

            @pl.when(zz != z)
            def _():
                remote(
                    zsend.at[zz], zbuf.at[z], z_send.at[zz], z_recv.at[z], zz * nq + q, t
                ).start()

    other = 1 - half
    shares(half, 0)
    remote(pbuf.at[other], pbuf.at[other], p_send, p_recv, me, partner).wait_recv()
    shares(other, 1)
    combine(half, 0)
    combine(other, 1)
    low = zsend[z]
    for d in range(1, nz):
        zz = (z + d) % nz
        remote(zsend.at[z], zbuf.at[zz], z_send.at[zz], z_recv.at[zz], me, t).wait_recv()
        low += zbuf[zz]

    first_new = 0.8 * first_ref[...] + 0.2 * low
    second_new = 0.9 * second_ref[...] + 0.1 * low * low
    ubuf[me] = first_new / jnp.sqrt(second_new)
    first_out[...] = first_new
    second_out[...] = second_new
    started += gather(ubuf.at[me], ubuf, u_send, u_recv)

    if rr % 8 == 0:
        update = ubuf[...].reshape(rank, cols)
    else:
        for i in range(n):
            ufull[i * rr : (i + 1) * rr, :] = ubuf[i]
        update = ufull[...]
    squares = jnp.sum(update * update, axis=0, keepdims=True)
    total = jnp.sum(squares, axis=1, keepdims=True)
    sums[t] = jnp.broadcast_to(total, sums.shape[1:])
    for d in range(1, tp):
        copy = remote(sums.at[t], sums.at[t], s_send.at[d], s_recv.at[t], me, (t + d) % tp)
        copy.start()
        started.append(copy)

    high, low_bits = split2(update)
    step = jnp.dot(basis_ref[...], high, preferred_element_type=jnp.float32)
    step += jnp.dot(basis_ref[...], low_bits, preferred_element_type=jnp.float32)

    whole = sums[t][:1]
    for d in range(1, tp):
        c = (t + d) % tp
        remote(sums.at[c], sums.at[c], s_send.at[d], s_recv.at[c], me, c).wait_recv()
        whole += sums[c][:1]
    whole = whole / (rank * cols * tp)
    loads[2].wait()
    for i in range(cols // DQK):
        at = slice(i * DQK, (i + 1) * DQK)
        head = jnp.sum(squares[:, at], axis=1, keepdims=True) / (rank * DQK)
        factor = 1.0 / jnp.sqrt(head + whole)
        block = step[:, at] * factor
        step_ref[:, at] = block
        copy_ref[:, at] = (mv[:, at] + block).astype(jnp.bfloat16)

    for copy in started:
        copy.wait_send()
    for d in range(1, nz):
        zz = (z + d) % nz
        remote(zsend.at[zz], zbuf.at[z], z_send.at[zz], z_recv.at[z], zz * nq + q, t).wait_send()


def body(n, tp, inputs, query_cot, query_basis, query_master, query_first, query_second):
    nq = 1
    while nq * nq < n:
        nq *= 2
    nz = n // nq
    tokens, width = inputs.shape
    rows, rank = query_basis.shape
    rr, cols = query_first.shape
    f32, bf16 = jnp.float32, jnp.bfloat16
    dma = pltpu.SemaphoreType.DMA
    vmem = pl.BlockSpec(memory_space=pltpu.VMEM)
    hbm = pl.BlockSpec(memory_space=pl.ANY)
    return pl.pallas_call(
        functools.partial(kernel, n, nz, nq, tp),
        out_shape=(
            jax.ShapeDtypeStruct((rows, cols), f32),
            jax.ShapeDtypeStruct((rr, cols), f32),
            jax.ShapeDtypeStruct((rr, cols), f32),
            jax.ShapeDtypeStruct((rows, cols), bf16),
        ),
        in_specs=[hbm, hbm, vmem, hbm, vmem, vmem],
        out_specs=(vmem,) * 4,
        scratch_shapes=[
            pltpu.VMEM((tokens, width), bf16),
            pltpu.VMEM((tokens, cols), bf16),
            pltpu.VMEM((rows, cols), f32),
            pltpu.VMEM((n, rows, rank // 2), bf16),
            pltpu.VMEM((2, tokens, rank // 2), f32),
            pltpu.VMEM((nq, nz, rr, cols), f32),
            pltpu.VMEM((nq, nz, rr, cols), f32),
            pltpu.VMEM((nz, rr, cols), f32),
            pltpu.VMEM((nz, rr, cols), f32),
            pltpu.VMEM((n, rr, cols), f32),
            pltpu.VMEM((rank, cols), f32),
            pltpu.VMEM((tp, 8, 128), f32),
            dma((4,)),
            dma((nz + n,)), dma((n,)),
            dma, dma,
            dma((2, nq)), dma((2, nq)),
            dma((nz,)), dma((nz,)),
            dma((nz + n,)), dma((n,)),
            dma((tp,)), dma((tp,)),
        ],
        compiler_params=pltpu.CompilerParams(collective_id=0, has_side_effects=True),
    )(inputs, query_cot, query_basis, query_master, query_first, query_second)


def solution(mesh):
    placed = (
        P("fs", None),
        P("fs", "tp"),
        P("fs", None),
        P("fs", "tp"),
        P("fs", "tp"),
        P("fs", "tp"),
    )
    return jax.shard_map(
        functools.partial(body, mesh.shape["fs"], mesh.shape["tp"]),
        mesh=mesh,
        in_specs=placed,
        out_specs=(P("fs", "tp"),) * 4,
        check_vma=False,
    )
```

```python
import functools

import jax
import jax.numpy as jnp
from jax import lax
from jax.experimental import pallas as pl
from jax.experimental.pallas import tpu as pltpu
from jax.sharding import PartitionSpec as P

DQK = 128
MESH = pl.DeviceIdType.MESH
CONTRACT = (((0,), (0,)), ((), ()))


def split2(value):
    high = value.astype(jnp.bfloat16)
    low = (value - high.astype(jnp.float32)).astype(jnp.bfloat16)
    return high, low


def moments(first, second, low):
    return 0.8 * first + 0.2 * low, 0.9 * second + 0.1 * low * low


def kernel(
    n, nz, nq, tp,
    inputs_ref, cot_ref, basis_ref, first_ref, second_ref,
    product_ref, factor_ref, low_ref,
    xv, cv, bv, fv, sv, ball, pbuf, part, rbuf, zsend, zbuf, ubuf, ufull, sums,
    load_sem, b_send, b_recv, p_send, p_recv, r_send, r_recv, z_send, z_recv,
    u_send, u_recv, s_send, s_recv,
):
    me = lax.axis_index("fs")
    t = lax.axis_index("tp")
    z, q = me // nq, me % nq
    half = t % 2
    partner = t + 1 - 2 * half
    rank_half = ball.shape[2]
    rr, cols = first_ref.shape
    rank = rr * n
    nzh = nz // 2

    def remote(src, dst, send, recv, fs, core):
        return pltpu.make_async_remote_copy(
            src_ref=src, dst_ref=dst, send_sem=send, recv_sem=recv,
            device_id=(fs, core), device_id_type=MESH,
        )

    own_basis = basis_ref.at[:, pl.ds(pl.multiple_of(half * rank_half, rank_half), rank_half)]
    loads = [
        pltpu.make_async_copy(own_basis, ball.at[me], load_sem.at[0]),
        pltpu.make_async_copy(inputs_ref, xv, load_sem.at[1]),
        pltpu.make_async_copy(cot_ref, cv, load_sem.at[2]),
        pltpu.make_async_copy(first_ref, fv, load_sem.at[3]),
        pltpu.make_async_copy(second_ref, sv, load_sem.at[4]),
        pltpu.make_async_copy(basis_ref, bv, load_sem.at[5]),
    ]

    barrier = pltpu.get_barrier_semaphore()
    for d in range(1, nz):
        pl.semaphore_signal(barrier, inc=1, device_id=((z + d) % nz * nq + q, t), device_id_type=MESH)
    for d in range(1, nq):
        pl.semaphore_signal(barrier, inc=1, device_id=(z * nq + (q + d) % nq, t), device_id_type=MESH)
    for d in range(1, tp):
        pl.semaphore_signal(barrier, inc=1, device_id=(me, (t + d) % tp), device_id_type=MESH)
    for load in loads:
        load.start()
    pl.semaphore_wait(barrier, nz - 1 + nq - 1 + tp - 1)

    def gather(own, buf, send, recv):
        started = []
        for d in range(1, nz):
            copy = remote(own, buf.at[me], send.at[d], recv.at[me], (z + d) % nz * nq + q, t)
            copy.start()
            started.append(copy)
        for k in range(nz):
            c = (z + k) % nz * nq + q
            if k > 0:
                remote(own, buf.at[c], send.at[0], recv.at[c], me, t).wait_recv()
            source = own if k == 0 else buf.at[c]
            for d in range(1, nq):
                copy = remote(
                    source, buf.at[c], send.at[nz + k * nq + d], recv.at[c], z * nq + (q + d) % nq, t
                )
                copy.start()
                started.append(copy)
        for k in range(nz):
            for d in range(1, nq):
                c = (z + k) % nz * nq + (q + d) % nq
                remote(own, buf.at[c], send.at[0], recv.at[c], me, t).wait_recv()
        return started

    started = []
    loads[0].wait()
    started += gather(ball.at[me], ball, b_send, b_recv)

    loads[1].wait()
    pbuf[half] = jnp.dot(
        xv[...], ball[...].reshape(xv.shape[1], rank_half), preferred_element_type=jnp.float32
    )
    swap = remote(pbuf.at[half], pbuf.at[half], p_send, p_recv, me, partner)
    swap.start()
    started.append(swap)
    loads[2].wait()

    def shares(hh, slot):
        high, low = split2(pbuf[hh])
        value = lax.dot_general(high, cv[...], CONTRACT, preferred_element_type=jnp.float32)
        value += lax.dot_general(low, cv[...], CONTRACT, preferred_element_type=jnp.float32)
        for k in range(nzh):
            for j in range(nq):
                at = (k * nq + j) * rr
                part[j, hh * nzh + k] = value[at : at + rr].astype(part.dtype)
        for d in range(1, nq):
            to = (q + d) % nq
            copy = remote(
                part.at[to, pl.ds(hh * nzh, nzh)], rbuf.at[q, pl.ds(hh * nzh, nzh)],
                r_send.at[slot, d], r_recv.at[slot, q], z * nq + to, t,
            )
            copy.start()
            started.append(copy)

    def combine(hh, slot):
        for d in range(1, nq):
            j = (q + d) % nq
            remote(
                part.at[j, pl.ds(hh * nzh, nzh)], rbuf.at[j, pl.ds(hh * nzh, nzh)],
                r_send.at[slot, 0], r_recv.at[slot, j], me, t,
            ).wait_recv()
        for k in range(nzh):
            zz = hh * nzh + k
            total = part[q, zz].astype(jnp.float32)
            for d in range(1, nq):
                total += rbuf[(q + d) % nq, zz].astype(jnp.float32)
            zsend[zz] = total

            @pl.when(zz != z)
            def _():
                remote(
                    zsend.at[zz], zbuf.at[z], z_send.at[zz], z_recv.at[z], zz * nq + q, t
                ).start()

    other = 1 - half
    shares(half, 0)
    remote(pbuf.at[other], pbuf.at[other], p_send, p_recv, me, partner).wait_recv()
    shares(other, 1)
    combine(half, 0)
    combine(other, 1)
    low = zsend[z]
    for d in range(1, nz):
        zz = (z + d) % nz
        remote(zsend.at[z], zbuf.at[zz], z_send.at[zz], z_recv.at[zz], me, t).wait_recv()
        low += zbuf[zz]

    for load in loads[3:]:
        load.wait()
    first_new, second_new = moments(fv[...], sv[...], low)
    ubuf[me] = first_new / jnp.sqrt(second_new)
    low_ref[...] = low
    started += gather(ubuf.at[me], ubuf, u_send, u_recv)

    if rr % 8 == 0:
        update = ubuf[...].reshape(rank, cols)
    else:
        for i in range(n):
            ufull[i * rr : (i + 1) * rr, :] = ubuf[i]
        update = ufull[...]
    squares = jnp.sum(update * update, axis=0, keepdims=True)
    total = jnp.sum(squares, axis=1, keepdims=True)
    sums[t] = jnp.broadcast_to(total, sums.shape[1:])
    for d in range(1, tp):
        copy = remote(sums.at[t], sums.at[t], s_send.at[d], s_recv.at[t], me, (t + d) % tp)
        copy.start()
        started.append(copy)

    high, low_bits = split2(update)
    product = jnp.dot(bv[...], high, preferred_element_type=jnp.float32)
    product += jnp.dot(bv[...], low_bits, preferred_element_type=jnp.float32)
    product_ref[...] = product

    whole = sums[t][:1]
    for d in range(1, tp):
        c = (t + d) % tp
        remote(sums.at[c], sums.at[c], s_send.at[d], s_recv.at[c], me, c).wait_recv()
        whole += sums[c][:1]
    whole = whole / (rank * cols * tp)
    for i in range(cols // DQK):
        at = slice(i * DQK, (i + 1) * DQK)
        head = jnp.sum(squares[:, at], axis=1, keepdims=True) / (rank * DQK)
        factor = 1.0 / jnp.sqrt(head + whole)
        factor_ref[:, at] = jnp.broadcast_to(factor, (factor_ref.shape[0], DQK))

    for copy in started:
        copy.wait_send()
    for d in range(1, nz):
        zz = (z + d) % nz
        remote(zsend.at[zz], zbuf.at[z], z_send.at[zz], z_recv.at[z], zz * nq + q, t).wait_send()


def finish(
    product_ref, factor_ref, low_ref, first_ref, second_ref, master_ref,
    step_ref, first_out, second_out, copy_ref,
):
    first_out[...], second_out[...] = moments(first_ref[...], second_ref[...], low_ref[...])
    step = product_ref[...] * factor_ref[:1]
    step_ref[...] = step
    copy_ref[...] = (master_ref[...] + step).astype(jnp.bfloat16)


def body(n, tp, inputs, query_cot, query_basis, query_master, query_first, query_second):
    nq = 1
    while nq * nq < n:
        nq *= 2
    nz = n // nq
    tokens, width = inputs.shape
    rows, rank = query_basis.shape
    rr, cols = query_first.shape
    f32, bf16 = jnp.float32, jnp.bfloat16
    dma = pltpu.SemaphoreType.DMA
    vmem = pl.BlockSpec(memory_space=pltpu.VMEM)
    hbm = pl.BlockSpec(memory_space=pl.ANY)
    product, factor, low = pl.pallas_call(
        functools.partial(kernel, n, nz, nq, tp),
        out_shape=(
            jax.ShapeDtypeStruct((rows, cols), f32),
            jax.ShapeDtypeStruct((8, cols), f32),
            jax.ShapeDtypeStruct((rr, cols), f32),
        ),
        in_specs=[hbm] * 5,
        out_specs=(vmem,) * 3,
        scratch_shapes=[
            pltpu.VMEM((tokens, width), bf16),
            pltpu.VMEM((tokens, cols), bf16),
            pltpu.VMEM((rows, rank), bf16),
            pltpu.VMEM((rr, cols), f32),
            pltpu.VMEM((rr, cols), f32),
            pltpu.VMEM((n, rows, rank // 2), bf16),
            pltpu.VMEM((2, tokens, rank // 2), f32),
            pltpu.VMEM((nq, nz, rr, cols), f32),
            pltpu.VMEM((nq, nz, rr, cols), f32),
            pltpu.VMEM((nz, rr, cols), f32),
            pltpu.VMEM((nz, rr, cols), f32),
            pltpu.VMEM((n, rr, cols), f32),
            pltpu.VMEM((rank, cols), f32),
            pltpu.VMEM((tp, 8, 128), f32),
            dma((6,)),
            dma((nz + n,)), dma((n,)),
            dma, dma,
            dma((2, nq)), dma((2, nq)),
            dma((nz,)), dma((nz,)),
            dma((nz + n,)), dma((n,)),
            dma((tp,)), dma((tp,)),
        ],
        compiler_params=pltpu.CompilerParams(collective_id=0, has_side_effects=True),
    )(inputs, query_cot, query_basis, query_first, query_second)
    return pl.pallas_call(
        finish,
        out_shape=(
            jax.ShapeDtypeStruct((rows, cols), f32),
            jax.ShapeDtypeStruct((rr, cols), f32),
            jax.ShapeDtypeStruct((rr, cols), f32),
            jax.ShapeDtypeStruct((rows, cols), bf16),
        ),
        in_specs=[vmem] * 6,
        out_specs=(vmem,) * 4,
    )(product, factor, low, query_first, query_second, query_master)


def solution(mesh):
    placed = (
        P("fs", None),
        P("fs", "tp"),
        P("fs", None),
        P("fs", "tp"),
        P("fs", "tp"),
        P("fs", "tp"),
    )
    return jax.shard_map(
        functools.partial(body, mesh.shape["fs"], mesh.shape["tp"]),
        mesh=mesh,
        in_specs=placed,
        out_specs=(P("fs", "tp"),) * 4,
        check_vma=False,
    )
```

```python
import functools

import jax
import jax.numpy as jnp
from jax import lax
from jax.experimental import pallas as pl
from jax.experimental.pallas import tpu as pltpu
from jax.sharding import PartitionSpec as P

DQK = 128
MESH = pl.DeviceIdType.MESH
CONTRACT = (((0,), (0,)), ((), ()))


def split2(value):
    high = value.astype(jnp.bfloat16)
    low = (value - high.astype(jnp.float32)).astype(jnp.bfloat16)
    return high, low


def moments(first, second, low):
    return 0.8 * first + 0.2 * low, 0.9 * second + 0.1 * low * low


def kernel(
    n, na, nb, nz, tp, groups,
    inputs_ref, cot_ref, basis_ref, first_ref, second_ref,
    product_ref, factor_ref, low_ref,
    xv, cv, bv, fv, sv, ball, pbuf, part, rbuf, zsend, zbuf, ubuf, ufull, sums,
    load_sem, send_sem, p_recv, b_recv, r_recv, z_send, z_recv, u_recv, s_recv,
):
    me = lax.axis_index("fs")
    t = lax.axis_index("tp")
    nq = na * nb
    z, q = me // nq, me % nq
    a, b = q // nb, q % nb
    half = t % 2
    partner = t + 1 - 2 * half
    rank_half = bv.shape[1] // 2
    rows = bv.shape[0]
    rr, cols = first_ref.shape
    rank = rr * n
    nzh = nz // 2
    width = cols // groups
    started = []

    def remote(src, dst, send, recv, fs, core):
        return pltpu.make_async_remote_copy(
            src_ref=src, dst_ref=dst, send_sem=send, recv_sem=recv,
            device_id=(fs, core), device_id_type=MESH,
        )

    def send(src, dst, recv, fs, core):
        copy = remote(src, dst, send_sem.at[len(started)], recv, fs, core)
        copy.start()
        started.append(copy)

    def arrive(dst, recv):
        remote(dst, dst, send_sem.at[0], recv, me, t).wait_recv()

    def at(zz, aa, bb):
        return (zz * na + aa) * nb + bb

    own_basis = basis_ref.at[:, pl.ds(pl.multiple_of(half * rank_half, rank_half), rank_half)]
    loads = [
        pltpu.make_async_copy(own_basis.at[: rows // 2], ball.at[me, 0], load_sem.at[0]),
        pltpu.make_async_copy(own_basis.at[rows // 2 :], ball.at[me, 1], load_sem.at[1]),
        pltpu.make_async_copy(inputs_ref, xv, load_sem.at[2]),
        pltpu.make_async_copy(cot_ref, cv, load_sem.at[3]),
        pltpu.make_async_copy(first_ref, fv, load_sem.at[4]),
        pltpu.make_async_copy(second_ref, sv, load_sem.at[5]),
        pltpu.make_async_copy(basis_ref, bv, load_sem.at[6]),
    ]

    barrier = pltpu.get_barrier_semaphore()
    for d in range(1, nz):
        pl.semaphore_signal(barrier, inc=1, device_id=((z + d) % nz * nq + q, t), device_id_type=MESH)
    for d in range(1, nq):
        pl.semaphore_signal(barrier, inc=1, device_id=(z * nq + (q + d) % nq, t), device_id_type=MESH)
    for d in range(1, tp):
        pl.semaphore_signal(barrier, inc=1, device_id=(me, (t + d) % tp), device_id_type=MESH)
    for load in loads:
        load.start()
    pl.semaphore_wait(barrier, nz - 1 + nq - 1 + tp - 1)

    class Gather:
        def __init__(self, view, recv, order):
            self.view, self.recv, self.order = view, recv, order

        def pass_on(self, c, fs):
            send(self.view(c), self.view(c), self.recv.at[c], fs, t)

        def near(self, k):
            c = at((z + k) % nz, a, b)
            if k > 0:
                arrive(self.view(c), self.recv.at[c])
            for d in range(1, na):
                self.pass_on(c, at(z, (a + d) % na, b))
            for d in range(1, nb):
                self.pass_on(c, at(z, a, (b + d) % nb))

        def begin(self):
            for d in range(1, nz):
                self.pass_on(me, at((z + d) % nz, a, b))
            self.near(0)

        def across(self, k):
            zz = (z + k) % nz
            if self.order == 0:
                for d in range(1, na):
                    c = at(zz, (a + d) % na, b)
                    arrive(self.view(c), self.recv.at[c])
                    for e in range(1, nb):
                        self.pass_on(c, at(z, a, (b + e) % nb))
            else:
                for e in range(1, nb):
                    c = at(zz, a, (b + e) % nb)
                    arrive(self.view(c), self.recv.at[c])
                    for d in range(1, na):
                        self.pass_on(c, at(z, (a + d) % na, b))

        def end(self, k):
            zz = (z + k) % nz
            for d in range(na):
                for e in range(nb):
                    seen = e == 0 if self.order == 0 else d == 0
                    if not seen:
                        c = at(zz, (a + d) % na, (b + e) % nb)
                        arrive(self.view(c), self.recv.at[c])

        def middle(self):
            for k in range(1, nz):
                self.near(k)
                self.across(k - 1)
            self.across(nz - 1)

    pieces = [
        Gather(lambda c, i=i: ball.at[c, i], b_recv.at[i], i) for i in range(2)
    ]
    loads[0].wait()
    loads[1].wait()
    for piece in pieces:
        piece.begin()
    for k in range(1, nz + 1):
        for piece in pieces:
            if k < nz:
                piece.near(k)
        for piece in pieces:
            piece.across(k - 1)
    loads[2].wait()
    projected = jnp.zeros((xv.shape[0], rank_half), jnp.float32)
    for k in range(nz):
        for piece in pieces:
            piece.end(k)
        zz = (z + k) % nz
        depth = nq * rows
        projected += jnp.dot(
            xv[:, pl.ds(pl.multiple_of(zz * depth, depth), depth)],
            ball[pl.ds(zz * nq, nq)].reshape(depth, rank_half),
            preferred_element_type=jnp.float32,
        )
    pbuf[half] = projected
    send(pbuf.at[half], pbuf.at[half], p_recv, me, partner)
    loads[3].wait()

    def shares(hh, slot, g):
        high, low = split2(pbuf[hh])
        cot = cv[:, g * width : (g + 1) * width]
        value = lax.dot_general(high, cot, CONTRACT, preferred_element_type=jnp.float32)
        value += lax.dot_general(low, cot, CONTRACT, preferred_element_type=jnp.float32)
        for k in range(nzh):
            for j in range(nq):
                row = (k * nq + j) * rr
                part[g, j, hh * nzh + k] = value[row : row + rr]
        for d in range(1, nq):
            to = (q + d) % nq
            send(
                part.at[g, to, pl.ds(hh * nzh, nzh)], rbuf.at[g, q, pl.ds(hh * nzh, nzh)],
                r_recv.at[g, slot, q], z * nq + to, t,
            )

    def combine(hh, slot, g):
        for d in range(1, nq):
            j = (q + d) % nq
            arrive(rbuf.at[g, j, pl.ds(hh * nzh, nzh)], r_recv.at[g, slot, j])
        for k in range(nzh):
            zz = hh * nzh + k
            total = part[g, q, zz]
            for d in range(1, nq):
                total += rbuf[g, (q + d) % nq, zz]
            zsend[g, zz] = total

            @pl.when(zz != z)
            def _():
                remote(
                    zsend.at[g, zz], zbuf.at[g, z], z_send.at[g, zz], z_recv.at[g, z], zz * nq + q, t
                ).start()

    def settle(g):
        low = zsend[g, z]
        for d in range(1, nz):
            zz = (z + d) % nz
            arrive(zbuf.at[g, zz], z_recv.at[g, zz])
            low += zbuf[g, zz]
        if g == 0:
            for load in loads[4:]:
                load.wait()
        here = slice(g * width, (g + 1) * width)
        first_new, second_new = moments(fv[:, here], sv[:, here], low)
        ubuf[g, me] = first_new / jnp.sqrt(second_new)
        low_ref[:, here] = low

    other = 1 - half
    updates = [
        Gather(lambda c, g=g: ubuf.at[g, c], u_recv.at[g], g % 2) for g in range(groups)
    ]
    for g in range(groups):
        shares(half, 0, g)
        if g == 0:
            arrive(pbuf.at[other], p_recv)
        shares(other, 1, g)
    for g in range(groups):
        combine(half, 0, g)
        if g > 0:
            settle(g - 1)
            updates[g - 1].begin()
        combine(other, 1, g)
        if g > 0:
            updates[g - 1].middle()
    settle(groups - 1)
    updates[groups - 1].begin()
    updates[groups - 1].middle()

    squares = []
    for g in range(groups):
        for k in range(nz):
            updates[g].end(k)
        if rr % 8 == 0:
            update = ubuf[g].reshape(rank, width)
        else:
            for i in range(n):
                ufull[i * rr : (i + 1) * rr, :] = ubuf[g, i]
            update = ufull[...]
        squares.append(jnp.sum(update * update, axis=0, keepdims=True))
        if g == groups - 1:
            total = sum(jnp.sum(x, axis=1, keepdims=True) for x in squares)
            sums[t] = jnp.broadcast_to(total, sums.shape[1:])
            for d in range(1, tp):
                send(sums.at[t], sums.at[t], s_recv.at[t], me, (t + d) % tp)
        high, rest = split2(update)
        product = jnp.dot(bv[...], high, preferred_element_type=jnp.float32)
        product += jnp.dot(bv[...], rest, preferred_element_type=jnp.float32)
        product_ref[:, g * width : (g + 1) * width] = product

    whole = sums[t][:1]
    for d in range(1, tp):
        c = (t + d) % tp
        arrive(sums.at[c], s_recv.at[c])
        whole += sums[c][:1]
    whole = whole / (rank * cols * tp)
    for g in range(groups):
        for i in range(width // DQK):
            head = jnp.sum(squares[g][:, i * DQK : (i + 1) * DQK], axis=1, keepdims=True)
            factor = 1.0 / jnp.sqrt(head / (rank * DQK) + whole)
            spot = slice(g * width + i * DQK, g * width + (i + 1) * DQK)
            factor_ref[:, spot] = jnp.broadcast_to(factor, (factor_ref.shape[0], DQK))

    for copy in started:
        copy.wait_send()
    for g in range(groups):
        for d in range(1, nz):
            zz = (z + d) % nz
            remote(
                zsend.at[g, zz], zbuf.at[g, z], z_send.at[g, zz], z_recv.at[g, z], zz * nq + q, t
            ).wait_send()


def finish(
    product_ref, factor_ref, low_ref, first_ref, second_ref, master_ref,
    step_ref, first_out, second_out, copy_ref,
):
    first_out[...], second_out[...] = moments(first_ref[...], second_ref[...], low_ref[...])
    step = product_ref[...] * factor_ref[:1]
    step_ref[...] = step
    copy_ref[...] = (master_ref[...] + step).astype(jnp.bfloat16)


def body(n, tp, inputs, query_cot, query_basis, query_master, query_first, query_second):
    nq = 1
    while nq * nq < n:
        nq *= 2
    nz = n // nq
    na = min(2, nq)
    nb = nq // na
    tokens, width = inputs.shape
    rows, rank = query_basis.shape
    rr, cols = query_first.shape
    groups = 2 if cols % (2 * DQK) == 0 else 1
    width_g = cols // groups
    sends = (2 + groups) * (nz + nz * nq) + 2 * groups * nq + tp
    f32, bf16 = jnp.float32, jnp.bfloat16
    dma = pltpu.SemaphoreType.DMA
    vmem = pl.BlockSpec(memory_space=pltpu.VMEM)
    hbm = pl.BlockSpec(memory_space=pl.ANY)
    product, factor, low = pl.pallas_call(
        functools.partial(kernel, n, na, nb, nz, tp, groups),
        out_shape=(
            jax.ShapeDtypeStruct((rows, cols), f32),
            jax.ShapeDtypeStruct((8, cols), f32),
            jax.ShapeDtypeStruct((rr, cols), f32),
        ),
        in_specs=[hbm] * 5,
        out_specs=(vmem,) * 3,
        scratch_shapes=[
            pltpu.VMEM((tokens, width), bf16),
            pltpu.VMEM((tokens, cols), bf16),
            pltpu.VMEM((rows, rank), bf16),
            pltpu.VMEM((rr, cols), f32),
            pltpu.VMEM((rr, cols), f32),
            pltpu.VMEM((n, 2, rows // 2, rank // 2), bf16),
            pltpu.VMEM((2, tokens, rank // 2), f32),
            pltpu.VMEM((groups, nq, nz, rr, width_g), f32),
            pltpu.VMEM((groups, nq, nz, rr, width_g), f32),
            pltpu.VMEM((groups, nz, rr, width_g), f32),
            pltpu.VMEM((groups, nz, rr, width_g), f32),
            pltpu.VMEM((groups, n, rr, width_g), f32),
            pltpu.VMEM((rank, width_g), f32),
            pltpu.VMEM((tp, 8, 128), f32),
            dma((7,)), dma((sends,)),
            dma, dma((2, n)), dma((groups, 2, nq)),
            dma((groups, nz)), dma((groups, nz)),
            dma((groups, n)), dma((tp,)),
        ],
        compiler_params=pltpu.CompilerParams(collective_id=0, has_side_effects=True),
    )(inputs, query_cot, query_basis, query_first, query_second)
    return pl.pallas_call(
        finish,
        out_shape=(
            jax.ShapeDtypeStruct((rows, cols), f32),
            jax.ShapeDtypeStruct((rr, cols), f32),
            jax.ShapeDtypeStruct((rr, cols), f32),
            jax.ShapeDtypeStruct((rows, cols), bf16),
        ),
        in_specs=[vmem] * 6,
        out_specs=(vmem,) * 4,
    )(product, factor, low, query_first, query_second, query_master)


def solution(mesh):
    placed = (
        P("fs", None),
        P("fs", "tp"),
        P("fs", None),
        P("fs", "tp"),
        P("fs", "tp"),
        P("fs", "tp"),
    )
    return jax.shard_map(
        functools.partial(body, mesh.shape["fs"], mesh.shape["tp"]),
        mesh=mesh,
        in_specs=placed,
        out_specs=(P("fs", "tp"),) * 4,
        check_vma=False,
    )
```

```python
import functools

import jax
import jax.numpy as jnp
from jax import lax
from jax.experimental import pallas as pl
from jax.experimental.pallas import tpu as pltpu
from jax.sharding import PartitionSpec as P

DQK = 128
MESH = pl.DeviceIdType.MESH
CONTRACT = (((0,), (0,)), ((), ()))


def split2(value):
    high = value.astype(jnp.bfloat16)
    low = (value - high.astype(jnp.float32)).astype(jnp.bfloat16)
    return high, low


def moments(first, second, low):
    return 0.8 * first + 0.2 * low, 0.9 * second + 0.1 * low * low


def kernel(
    n, na, nb, nz, tp, groups,
    inputs_ref, cot_ref, basis_ref, first_ref, second_ref,
    product_ref, factor_ref, low_ref,
    xv, cv, bv, fv, sv, ball, pbuf, part, rbuf, zsend, zbuf, ubuf, ufull, sums,
    load_sem, send_sem, p_recv, b_recv, r_recv, z_send, z_recv, u_recv, s_recv,
):
    me = lax.axis_index("fs")
    t = lax.axis_index("tp")
    nq = na * nb
    z, q = me // nq, me % nq
    a, b = q // nb, q % nb
    half = t % 2
    partner = t + 1 - 2 * half
    rank_half = bv.shape[1] // 2
    rows = bv.shape[0]
    rr, cols = first_ref.shape
    rank = rr * n
    nzh = nz // 2
    width = cols // groups
    started = []

    def remote(src, dst, send, recv, fs, core):
        return pltpu.make_async_remote_copy(
            src_ref=src, dst_ref=dst, send_sem=send, recv_sem=recv,
            device_id=(fs, core), device_id_type=MESH,
        )

    def send(src, dst, recv, fs, core):
        copy = remote(src, dst, send_sem.at[len(started)], recv, fs, core)
        copy.start()
        started.append(copy)

    def arrive(dst, recv):
        remote(dst, dst, send_sem.at[0], recv, me, t).wait_recv()

    def at(zz, aa, bb):
        return (zz * na + aa) * nb + bb

    own_basis = basis_ref.at[:, pl.ds(pl.multiple_of(half * rank_half, rank_half), rank_half)]
    loads = [
        pltpu.make_async_copy(own_basis.at[: rows // 2], ball.at[me, 0], load_sem.at[0]),
        pltpu.make_async_copy(own_basis.at[rows // 2 :], ball.at[me, 1], load_sem.at[1]),
        pltpu.make_async_copy(inputs_ref, xv, load_sem.at[2]),
        pltpu.make_async_copy(cot_ref, cv, load_sem.at[3]),
        pltpu.make_async_copy(first_ref, fv, load_sem.at[4]),
        pltpu.make_async_copy(second_ref, sv, load_sem.at[5]),
        pltpu.make_async_copy(basis_ref, bv, load_sem.at[6]),
    ]

    barrier = pltpu.get_barrier_semaphore()
    for d in range(1, nz):
        pl.semaphore_signal(barrier, inc=1, device_id=((z + d) % nz * nq + q, t), device_id_type=MESH)
    for d in range(1, nq):
        pl.semaphore_signal(barrier, inc=1, device_id=(z * nq + (q + d) % nq, t), device_id_type=MESH)
    for d in range(1, tp):
        pl.semaphore_signal(barrier, inc=1, device_id=(me, (t + d) % tp), device_id_type=MESH)
    for load in loads:
        load.start()
    pl.semaphore_wait(barrier, nz - 1 + nq - 1 + tp - 1)

    class Gather:
        def __init__(self, view, recv, order):
            self.view, self.recv, self.order = view, recv, order

        def pass_on(self, c, fs):
            send(self.view(c), self.view(c), self.recv.at[c], fs, t)

        def near(self, k):
            c = at((z + k) % nz, a, b)
            if k > 0:
                arrive(self.view(c), self.recv.at[c])
            for d in range(1, nq):
                self.pass_on(c, z * nq + (q + d) % nq)

        def begin(self):
            for d in range(1, nz):
                self.pass_on(me, at((z + d) % nz, a, b))
            self.near(0)

        def across(self, k):
            pass

        def end(self, k):
            zz = (z + k) % nz
            for d in range(na):
                for e in range(nb):
                    seen = d == 0 and e == 0
                    if not seen:
                        c = at(zz, (a + d) % na, (b + e) % nb)
                        arrive(self.view(c), self.recv.at[c])

        def middle(self):
            for k in range(1, nz):
                self.near(k)
                self.across(k - 1)
            self.across(nz - 1)

    pieces = [
        Gather(lambda c, i=i: ball.at[c, i], b_recv.at[i], i) for i in range(2)
    ]
    loads[0].wait()
    loads[1].wait()
    for piece in pieces:
        piece.begin()
    for k in range(1, nz + 1):
        for piece in pieces:
            if k < nz:
                piece.near(k)
        for piece in pieces:
            piece.across(k - 1)
    loads[2].wait()
    projected = jnp.zeros((xv.shape[0], rank_half), jnp.float32)
    for k in range(nz):
        for piece in pieces:
            piece.end(k)
        zz = (z + k) % nz
        depth = nq * rows
        projected += jnp.dot(
            xv[:, pl.ds(pl.multiple_of(zz * depth, depth), depth)],
            ball[pl.ds(zz * nq, nq)].reshape(depth, rank_half),
            preferred_element_type=jnp.float32,
        )
    pbuf[half] = projected
    send(pbuf.at[half], pbuf.at[half], p_recv, me, partner)
    loads[3].wait()

    def shares(hh, slot, g):
        high, low = split2(pbuf[hh])
        cot = cv[:, g * width : (g + 1) * width]
        value = lax.dot_general(high, cot, CONTRACT, preferred_element_type=jnp.float32)
        value += lax.dot_general(low, cot, CONTRACT, preferred_element_type=jnp.float32)
        for k in range(nzh):
            for j in range(nq):
                row = (k * nq + j) * rr
                part[g, j, hh * nzh + k] = value[row : row + rr]
        for d in range(1, nq):
            to = (q + d) % nq
            send(
                part.at[g, to, pl.ds(hh * nzh, nzh)], rbuf.at[g, q, pl.ds(hh * nzh, nzh)],
                r_recv.at[g, slot, q], z * nq + to, t,
            )

    def combine(hh, slot, g):
        for d in range(1, nq):
            j = (q + d) % nq
            arrive(rbuf.at[g, j, pl.ds(hh * nzh, nzh)], r_recv.at[g, slot, j])
        for k in range(nzh):
            zz = hh * nzh + k
            total = part[g, q, zz]
            for d in range(1, nq):
                total += rbuf[g, (q + d) % nq, zz]
            zsend[g, zz] = total

            @pl.when(zz != z)
            def _():
                remote(
                    zsend.at[g, zz], zbuf.at[g, z], z_send.at[g, zz], z_recv.at[g, z], zz * nq + q, t
                ).start()

    def settle(g):
        low = zsend[g, z]
        for d in range(1, nz):
            zz = (z + d) % nz
            arrive(zbuf.at[g, zz], z_recv.at[g, zz])
            low += zbuf[g, zz]
        if g == 0:
            for load in loads[4:]:
                load.wait()
        here = slice(g * width, (g + 1) * width)
        first_new, second_new = moments(fv[:, here], sv[:, here], low)
        ubuf[g, me] = first_new / jnp.sqrt(second_new)
        low_ref[:, here] = low

    other = 1 - half
    updates = [
        Gather(lambda c, g=g: ubuf.at[g, c], u_recv.at[g], g % 2) for g in range(groups)
    ]
    for g in range(groups):
        shares(half, 0, g)
        if g == 0:
            arrive(pbuf.at[other], p_recv)
        shares(other, 1, g)
    for g in range(groups):
        combine(half, 0, g)
        if g > 0:
            settle(g - 1)
            updates[g - 1].begin()
        combine(other, 1, g)
        if g > 0:
            updates[g - 1].middle()
    settle(groups - 1)
    updates[groups - 1].begin()
    updates[groups - 1].middle()

    squares = []
    for g in range(groups):
        for k in range(nz):
            updates[g].end(k)
        if rr % 8 == 0:
            update = ubuf[g].reshape(rank, width)
        else:
            for i in range(n):
                ufull[i * rr : (i + 1) * rr, :] = ubuf[g, i]
            update = ufull[...]
        squares.append(jnp.sum(update * update, axis=0, keepdims=True))
        if g == groups - 1:
            total = sum(jnp.sum(x, axis=1, keepdims=True) for x in squares)
            sums[t] = jnp.broadcast_to(total, sums.shape[1:])
            for d in range(1, tp):
                send(sums.at[t], sums.at[t], s_recv.at[t], me, (t + d) % tp)
        high, rest = split2(update)
        product = jnp.dot(bv[...], high, preferred_element_type=jnp.float32)
        product += jnp.dot(bv[...], rest, preferred_element_type=jnp.float32)
        product_ref[:, g * width : (g + 1) * width] = product

    whole = sums[t][:1]
    for d in range(1, tp):
        c = (t + d) % tp
        arrive(sums.at[c], s_recv.at[c])
        whole += sums[c][:1]
    whole = whole / (rank * cols * tp)
    for g in range(groups):
        for i in range(width // DQK):
            head = jnp.sum(squares[g][:, i * DQK : (i + 1) * DQK], axis=1, keepdims=True)
            factor = 1.0 / jnp.sqrt(head / (rank * DQK) + whole)
            spot = slice(g * width + i * DQK, g * width + (i + 1) * DQK)
            factor_ref[:, spot] = jnp.broadcast_to(factor, (factor_ref.shape[0], DQK))

    for copy in started:
        copy.wait_send()
    for g in range(groups):
        for d in range(1, nz):
            zz = (z + d) % nz
            remote(
                zsend.at[g, zz], zbuf.at[g, z], z_send.at[g, zz], z_recv.at[g, z], zz * nq + q, t
            ).wait_send()


def finish(
    product_ref, factor_ref, low_ref, first_ref, second_ref, master_ref,
    step_ref, first_out, second_out, copy_ref,
):
    first_out[...], second_out[...] = moments(first_ref[...], second_ref[...], low_ref[...])
    step = product_ref[...] * factor_ref[:1]
    step_ref[...] = step
    copy_ref[...] = (master_ref[...] + step).astype(jnp.bfloat16)


def body(n, tp, inputs, query_cot, query_basis, query_master, query_first, query_second):
    nq = 1
    while nq * nq < n:
        nq *= 2
    nz = n // nq
    na = min(2, nq)
    nb = nq // na
    tokens, width = inputs.shape
    rows, rank = query_basis.shape
    rr, cols = query_first.shape
    groups = 1
    width_g = cols // groups
    sends = (2 + groups) * (nz + nz * nq) + 2 * groups * nq + tp
    f32, bf16 = jnp.float32, jnp.bfloat16
    dma = pltpu.SemaphoreType.DMA
    vmem = pl.BlockSpec(memory_space=pltpu.VMEM)
    hbm = pl.BlockSpec(memory_space=pl.ANY)
    product, factor, low = pl.pallas_call(
        functools.partial(kernel, n, na, nb, nz, tp, groups),
        out_shape=(
            jax.ShapeDtypeStruct((rows, cols), f32),
            jax.ShapeDtypeStruct((8, cols), f32),
            jax.ShapeDtypeStruct((rr, cols), f32),
        ),
        in_specs=[hbm] * 5,
        out_specs=(vmem,) * 3,
        scratch_shapes=[
            pltpu.VMEM((tokens, width), bf16),
            pltpu.VMEM((tokens, cols), bf16),
            pltpu.VMEM((rows, rank), bf16),
            pltpu.VMEM((rr, cols), f32),
            pltpu.VMEM((rr, cols), f32),
            pltpu.VMEM((n, 2, rows // 2, rank // 2), bf16),
            pltpu.VMEM((2, tokens, rank // 2), f32),
            pltpu.VMEM((groups, nq, nz, rr, width_g), f32),
            pltpu.VMEM((groups, nq, nz, rr, width_g), f32),
            pltpu.VMEM((groups, nz, rr, width_g), f32),
            pltpu.VMEM((groups, nz, rr, width_g), f32),
            pltpu.VMEM((groups, n, rr, width_g), f32),
            pltpu.VMEM((rank, width_g), f32),
            pltpu.VMEM((tp, 8, 128), f32),
            dma((7,)), dma((sends,)),
            dma, dma((2, n)), dma((groups, 2, nq)),
            dma((groups, nz)), dma((groups, nz)),
            dma((groups, n)), dma((tp,)),
        ],
        compiler_params=pltpu.CompilerParams(collective_id=0, has_side_effects=True),
    )(inputs, query_cot, query_basis, query_first, query_second)
    return pl.pallas_call(
        finish,
        out_shape=(
            jax.ShapeDtypeStruct((rows, cols), f32),
            jax.ShapeDtypeStruct((rr, cols), f32),
            jax.ShapeDtypeStruct((rr, cols), f32),
            jax.ShapeDtypeStruct((rows, cols), bf16),
        ),
        in_specs=[vmem] * 6,
        out_specs=(vmem,) * 4,
    )(product, factor, low, query_first, query_second, query_master)


def solution(mesh):
    placed = (
        P("fs", None),
        P("fs", "tp"),
        P("fs", None),
        P("fs", "tp"),
        P("fs", "tp"),
        P("fs", "tp"),
    )
    return jax.shard_map(
        functools.partial(body, mesh.shape["fs"], mesh.shape["tp"]),
        mesh=mesh,
        in_specs=placed,
        out_specs=(P("fs", "tp"),) * 4,
        check_vma=False,
    )
```

```python
import functools

import jax
import jax.numpy as jnp
from jax import lax
from jax.experimental import pallas as pl
from jax.experimental.pallas import tpu as pltpu
from jax.sharding import PartitionSpec as P

DQK = 128
MESH = pl.DeviceIdType.MESH
CONTRACT = (((0,), (0,)), ((), ()))


def split2(value):
    high = value.astype(jnp.bfloat16)
    low = (value - high.astype(jnp.float32)).astype(jnp.bfloat16)
    return high, low


def moments(first, second, low):
    return 0.8 * first + 0.2 * low, 0.9 * second + 0.1 * low * low


def kernel(
    n, na, nb, nz, tp, groups,
    inputs_ref, cot_ref, basis_ref, first_ref, second_ref,
    product_ref, factor_ref, low_ref,
    xv, cv, bv, fv, sv, ball, pbuf, part, rbuf, zsend, zbuf, ubuf, ufull, uhigh, urest, sums,
    load_sem, send_sem, p_recv, b_recv, r_recv, z_send, z_recv, u_recv, s_recv,
):
    me = lax.axis_index("fs")
    t = lax.axis_index("tp")
    nq = na * nb
    z, q = me // nq, me % nq
    a, b = q // nb, q % nb
    half = t % 2
    partner = t + 1 - 2 * half
    rank_half = bv.shape[1] // 2
    rows = bv.shape[0]
    rr, cols = first_ref.shape
    rank = rr * n
    nzh = nz // 2
    width = cols // groups
    started = []

    def remote(src, dst, send, recv, fs, core):
        return pltpu.make_async_remote_copy(
            src_ref=src, dst_ref=dst, send_sem=send, recv_sem=recv,
            device_id=(fs, core), device_id_type=MESH,
        )

    def send(src, dst, recv, fs, core):
        copy = remote(src, dst, send_sem.at[len(started)], recv, fs, core)
        copy.start()
        started.append(copy)

    def arrive(dst, recv):
        remote(dst, dst, send_sem.at[0], recv, me, t).wait_recv()

    def at(zz, aa, bb):
        return (zz * na + aa) * nb + bb

    own_basis = basis_ref.at[:, pl.ds(pl.multiple_of(half * rank_half, rank_half), rank_half)]
    loads = [
        pltpu.make_async_copy(own_basis.at[: rows // 2], ball.at[me, 0], load_sem.at[0]),
        pltpu.make_async_copy(own_basis.at[rows // 2 :], ball.at[me, 1], load_sem.at[1]),
        pltpu.make_async_copy(inputs_ref, xv, load_sem.at[2]),
        pltpu.make_async_copy(cot_ref, cv, load_sem.at[3]),
        pltpu.make_async_copy(first_ref, fv, load_sem.at[4]),
        pltpu.make_async_copy(second_ref, sv, load_sem.at[5]),
        pltpu.make_async_copy(basis_ref, bv, load_sem.at[6]),
    ]

    barrier = pltpu.get_barrier_semaphore()
    for d in range(1, nz):
        pl.semaphore_signal(barrier, inc=1, device_id=((z + d) % nz * nq + q, t), device_id_type=MESH)
    for d in range(1, nq):
        pl.semaphore_signal(barrier, inc=1, device_id=(z * nq + (q + d) % nq, t), device_id_type=MESH)
    for d in range(1, tp):
        pl.semaphore_signal(barrier, inc=1, device_id=(me, (t + d) % tp), device_id_type=MESH)
    for load in loads:
        load.start()
    pl.semaphore_wait(barrier, nz - 1 + nq - 1 + tp - 1)

    class Gather:
        def __init__(self, view, recv, order):
            self.view, self.recv, self.order = view, recv, order

        def pass_on(self, c, fs):
            send(self.view(c), self.view(c), self.recv.at[c], fs, t)

        def near(self, k):
            c = at((z + k) % nz, a, b)
            if k > 0:
                arrive(self.view(c), self.recv.at[c])
            for d in range(1, nq):
                self.pass_on(c, z * nq + (q + d) % nq)

        def begin(self):
            for d in range(1, nz):
                self.pass_on(me, at((z + d) % nz, a, b))
            self.near(0)

        def across(self, k):
            pass

        def end(self, k):
            zz = (z + k) % nz
            for d in range(na):
                for e in range(nb):
                    seen = d == 0 and e == 0
                    if not seen:
                        c = at(zz, (a + d) % na, (b + e) % nb)
                        arrive(self.view(c), self.recv.at[c])

        def middle(self):
            for k in range(1, nz):
                self.near(k)
                self.across(k - 1)
            self.across(nz - 1)

    pieces = [
        Gather(lambda c, i=i: ball.at[c, i], b_recv.at[i], i) for i in range(2)
    ]
    loads[0].wait()
    loads[1].wait()
    for piece in pieces:
        piece.begin()
    for k in range(1, nz + 1):
        for piece in pieces:
            if k < nz:
                piece.near(k)
        for piece in pieces:
            piece.across(k - 1)
    loads[2].wait()
    projected = jnp.zeros((xv.shape[0], rank_half), jnp.float32)
    for k in range(nz):
        for piece in pieces:
            piece.end(k)
        zz = (z + k) % nz
        depth = nq * rows
        projected += jnp.dot(
            xv[:, pl.ds(pl.multiple_of(zz * depth, depth), depth)],
            ball[pl.ds(zz * nq, nq)].reshape(depth, rank_half),
            preferred_element_type=jnp.float32,
        )
    pbuf[half] = projected
    send(pbuf.at[half], pbuf.at[half], p_recv, me, partner)
    loads[3].wait()

    def shares(hh, slot, g):
        high, low = split2(pbuf[hh])
        cot = cv[:, g * width : (g + 1) * width]
        value = lax.dot_general(high, cot, CONTRACT, preferred_element_type=jnp.float32)
        value += lax.dot_general(low, cot, CONTRACT, preferred_element_type=jnp.float32)
        for k in range(nzh):
            for j in range(nq):
                row = (k * nq + j) * rr
                part[g, j, hh * nzh + k] = value[row : row + rr]
        for d in range(1, nq):
            to = (q + d) % nq
            send(
                part.at[g, to, pl.ds(hh * nzh, nzh)], rbuf.at[g, q, pl.ds(hh * nzh, nzh)],
                r_recv.at[g, slot, q], z * nq + to, t,
            )

    def combine(hh, slot, g):
        for d in range(1, nq):
            j = (q + d) % nq
            arrive(rbuf.at[g, j, pl.ds(hh * nzh, nzh)], r_recv.at[g, slot, j])
        for k in range(nzh):
            zz = hh * nzh + k
            total = part[g, q, zz]
            for d in range(1, nq):
                total += rbuf[g, (q + d) % nq, zz]
            zsend[g, zz] = total

            @pl.when(zz != z)
            def _():
                remote(
                    zsend.at[g, zz], zbuf.at[g, z], z_send.at[g, zz], z_recv.at[g, z], zz * nq + q, t
                ).start()

    def settle(g):
        low = zsend[g, z]
        for d in range(1, nz):
            zz = (z + d) % nz
            arrive(zbuf.at[g, zz], z_recv.at[g, zz])
            low += zbuf[g, zz]
        if g == 0:
            for load in loads[4:]:
                load.wait()
        here = slice(g * width, (g + 1) * width)
        first_new, second_new = moments(fv[:, here], sv[:, here], low)
        ubuf[g, me] = first_new / jnp.sqrt(second_new)
        low_ref[:, here] = low

    other = 1 - half
    updates = [
        Gather(lambda c, g=g: ubuf.at[g, c], u_recv.at[g], g % 2) for g in range(groups)
    ]
    for g in range(groups):
        shares(half, 0, g)
        if g == 0:
            arrive(pbuf.at[other], p_recv)
        shares(other, 1, g)
    for g in range(groups):
        combine(half, 0, g)
        if g > 0:
            settle(g - 1)
            updates[g - 1].begin()
        combine(other, 1, g)
        if g > 0:
            updates[g - 1].middle()
    settle(groups - 1)
    updates[groups - 1].begin()
    updates[groups - 1].middle()

    squares = []
    for g in range(groups):
        depth = nq * rr
        square = jnp.zeros((1, width), jnp.float32)
        for k in range(nz):
            updates[g].end(k)
            zz = (z + k) % nz
            if rr % 8 == 0:
                update = ubuf[g, pl.ds(zz * nq, nq)].reshape(depth, width)
            else:
                for i in range(nq):
                    ufull[i * rr : (i + 1) * rr, :] = ubuf[g, zz * nq + i]
                update = ufull[:depth, :]
            square += jnp.sum(update * update, axis=0, keepdims=True)
            spot = pl.ds(pl.multiple_of(zz * depth, depth), depth)
            uhigh[spot, :], urest[spot, :] = split2(update)
        squares.append(square)
        if g == groups - 1:
            total = sum(jnp.sum(x, axis=1, keepdims=True) for x in squares)
            sums[t] = jnp.broadcast_to(total, sums.shape[1:])
            for d in range(1, tp):
                send(sums.at[t], sums.at[t], s_recv.at[t], me, (t + d) % tp)
        product = jnp.dot(bv[...], uhigh[...], preferred_element_type=jnp.float32)
        product += jnp.dot(bv[...], urest[...], preferred_element_type=jnp.float32)
        product_ref[:, g * width : (g + 1) * width] = product

    whole = sums[t][:1]
    for d in range(1, tp):
        c = (t + d) % tp
        arrive(sums.at[c], s_recv.at[c])
        whole += sums[c][:1]
    whole = whole / (rank * cols * tp)
    for g in range(groups):
        for i in range(width // DQK):
            head = jnp.sum(squares[g][:, i * DQK : (i + 1) * DQK], axis=1, keepdims=True)
            factor = 1.0 / jnp.sqrt(head / (rank * DQK) + whole)
            spot = slice(g * width + i * DQK, g * width + (i + 1) * DQK)
            factor_ref[:, spot] = jnp.broadcast_to(factor, (factor_ref.shape[0], DQK))

    for copy in started:
        copy.wait_send()
    for g in range(groups):
        for d in range(1, nz):
            zz = (z + d) % nz
            remote(
                zsend.at[g, zz], zbuf.at[g, z], z_send.at[g, zz], z_recv.at[g, z], zz * nq + q, t
            ).wait_send()


def finish(
    product_ref, factor_ref, low_ref, first_ref, second_ref, master_ref,
    step_ref, first_out, second_out, copy_ref,
):
    first_out[...], second_out[...] = moments(first_ref[...], second_ref[...], low_ref[...])
    step = product_ref[...] * factor_ref[:1]
    step_ref[...] = step
    copy_ref[...] = (master_ref[...] + step).astype(jnp.bfloat16)


def body(n, tp, inputs, query_cot, query_basis, query_master, query_first, query_second):
    nq = 1
    while nq * nq < n:
        nq *= 2
    nz = n // nq
    na = min(2, nq)
    nb = nq // na
    tokens, width = inputs.shape
    rows, rank = query_basis.shape
    rr, cols = query_first.shape
    groups = 1
    width_g = cols // groups
    sends = (2 + groups) * (nz + nz * nq) + 2 * groups * nq + tp
    f32, bf16 = jnp.float32, jnp.bfloat16
    dma = pltpu.SemaphoreType.DMA
    vmem = pl.BlockSpec(memory_space=pltpu.VMEM)
    hbm = pl.BlockSpec(memory_space=pl.ANY)
    product, factor, low = pl.pallas_call(
        functools.partial(kernel, n, na, nb, nz, tp, groups),
        out_shape=(
            jax.ShapeDtypeStruct((rows, cols), f32),
            jax.ShapeDtypeStruct((8, cols), f32),
            jax.ShapeDtypeStruct((rr, cols), f32),
        ),
        in_specs=[hbm] * 5,
        out_specs=(vmem,) * 3,
        scratch_shapes=[
            pltpu.VMEM((tokens, width), bf16),
            pltpu.VMEM((tokens, cols), bf16),
            pltpu.VMEM((rows, rank), bf16),
            pltpu.VMEM((rr, cols), f32),
            pltpu.VMEM((rr, cols), f32),
            pltpu.VMEM((n, 2, rows // 2, rank // 2), bf16),
            pltpu.VMEM((2, tokens, rank // 2), f32),
            pltpu.VMEM((groups, nq, nz, rr, width_g), f32),
            pltpu.VMEM((groups, nq, nz, rr, width_g), f32),
            pltpu.VMEM((groups, nz, rr, width_g), f32),
            pltpu.VMEM((groups, nz, rr, width_g), f32),
            pltpu.VMEM((groups, n, rr, width_g), f32),
            pltpu.VMEM((rank, width_g), f32),
            pltpu.VMEM((rank, width_g), bf16),
            pltpu.VMEM((rank, width_g), bf16),
            pltpu.VMEM((tp, 8, 128), f32),
            dma((7,)), dma((sends,)),
            dma, dma((2, n)), dma((groups, 2, nq)),
            dma((groups, nz)), dma((groups, nz)),
            dma((groups, n)), dma((tp,)),
        ],
        compiler_params=pltpu.CompilerParams(collective_id=0, has_side_effects=True),
    )(inputs, query_cot, query_basis, query_first, query_second)
    return pl.pallas_call(
        finish,
        out_shape=(
            jax.ShapeDtypeStruct((rows, cols), f32),
            jax.ShapeDtypeStruct((rr, cols), f32),
            jax.ShapeDtypeStruct((rr, cols), f32),
            jax.ShapeDtypeStruct((rows, cols), bf16),
        ),
        in_specs=[vmem] * 6,
        out_specs=(vmem,) * 4,
    )(product, factor, low, query_first, query_second, query_master)


def solution(mesh):
    placed = (
        P("fs", None),
        P("fs", "tp"),
        P("fs", None),
        P("fs", "tp"),
        P("fs", "tp"),
        P("fs", "tp"),
    )
    return jax.shard_map(
        functools.partial(body, mesh.shape["fs"], mesh.shape["tp"]),
        mesh=mesh,
        in_specs=placed,
        out_specs=(P("fs", "tp"),) * 4,
        check_vma=False,
    )
```
